32 devices in a mesh: fs: 4 (over y, x), tp: 8 (over z, core).
Axes of the slice: x: 2, y: 2, z: 4, core: 2. Of those that a mesh axis runs over, the one named last changes fastest.
Arguments:
- stream_in: bfloat16 [4096, 4096], P(('fs', 'tp')), may hold values from -6 to 6
- mixer_out: bfloat16 [4096, 4096], P(('fs', 'tp')), may hold values from -6 to 6
- mix_gain: float32 [4096], replicated, may hold values from 0.1 to 1.9
- pre_gain: float32 [4096], replicated, may hold values from 0.1 to 1.9
- gate_weight: float32 [4096, 6144], P('fs', 'tp'), may hold values from -0.09375 to 0.09375
- up_weight: float32 [4096, 6144], P('fs', 'tp'), may hold values from -0.09375 to 0.09375
- gate_scale: float32 [6144], P('tp'), may hold values from 0.5 to 2
- up_scale: float32 [6144], P('tp'), may hold values from 0.5 to 2
Outputs:
- hidden: bfloat16 [4096, 6144], P('fs', 'tp')
- stream: bfloat16 [4096, 4096], P(('fs', 'tp'))
The draws below stay inside these ranges and needn't reach their ends.
All inputs are finite; a program needn't handle non-finite values.
Results may differ from the reference program's by a relative error of at most 0.0082.
Values may be sent and summed in bfloat16 or wider, within the bound.
A program may use at most 128 MiB of HBM per device.

```python
import math
import jax
import jax.numpy as jnp
from jax import lax

D = 4096
FF = 6144
TOKENS = 4096


def levels(rng, shape, split, low, largest):
    def one(dim, shards_of):
        steps = jax.random.uniform(jax.random.fold_in(jax.random.fold_in(rng, 6), dim), (shards_of,), jnp.float32, low / len(split), largest / len(split))
        return jnp.repeat(jnp.exp(steps), shape[dim] // shards_of).reshape((-1,) + (1,) * (len(shape) - dim - 1))

    level = one(*split[0])
    for cut in split[1:]:
        level = level * one(*cut)
    return level


def centred(key, extent, width, limit, pieces=(), kind=jnp.bfloat16):
    entries = jax.random.normal(key, extent, jnp.float32) * width
    if len(pieces) > 0:
        entries = levels(key, extent, pieces, -0.22, 0.18) * entries
    return jnp.clip(entries, min=-limit, max=limit).astype(kind)


def setup_inputs(seed: int = 0) -> dict:
    splits = jax.random.split(jax.random.key(seed), 9)
    stream_in = centred(splits[0], (TOKENS, D), 1.0, 6.0, ((0, 32),))
    mixer_out = centred(splits[1], (TOKENS, D), 1.0, 6.0, ((0, 32),))
    mix_gain = jnp.clip(1.0 + 0.18 * jax.random.normal(splits[2], (D,), jnp.float32), 0.1, 1.9)
    pre_gain = jnp.clip(1.0 + 0.18 * jax.random.normal(splits[3], (D,), jnp.float32), 0.1, 1.9)
    gate_weight = centred(splits[4], (D, FF), D ** -0.5, 0.09375, ((0, 4), (1, 8)), jnp.float32)
    up_weight = centred(splits[5], (D, FF), D ** -0.5, 0.09375, ((0, 4), (1, 8)), jnp.float32)
    gate_scale = jnp.clip(jnp.exp(math.log(2.0) - 1.3862944 * jax.random.uniform(splits[6], (FF,), jnp.float32) ** levels(splits[6], (FF,), ((0, 8),), -0.2, 0.2)), 0.5, 2.0)
    up_scale = jnp.clip(jnp.exp(math.log(2.0) - 1.3862944 * jax.random.uniform(splits[7], (FF,), jnp.float32) ** levels(splits[7], (FF,), ((0, 8),), -0.2, 0.2)), 0.5, 2.0)
    return {"stream_in": stream_in, "mixer_out": mixer_out, "mix_gain": mix_gain, "pre_gain": pre_gain, "gate_weight": gate_weight, "up_weight": up_weight, "gate_scale": gate_scale, "up_scale": up_scale}


epsilon = 1e-06

def rms_scaled(values, gain):
    return values * lax.rsqrt(lax.optimization_barrier(jnp.mean(values * values, axis=-1, keepdims=True)) + epsilon) * gain

def reference(stream_in, mixer_out, mix_gain, pre_gain, gate_weight, up_weight, gate_scale, up_scale):
    mixed = stream_in.astype(jnp.float32) + rms_scaled(mixer_out.astype(jnp.float32), mix_gain)
    stream = mixed.astype(jnp.bfloat16)
    normed = rms_scaled(stream.astype(jnp.float32), pre_gain).astype(jnp.bfloat16)
    gate = jnp.dot(normed, gate_weight.astype(jnp.bfloat16), preferred_element_type=jnp.float32) * gate_scale
    up = jnp.dot(normed, up_weight.astype(jnp.bfloat16), preferred_element_type=jnp.float32) * up_scale
    hidden = (jax.nn.silu(gate) * up).astype(jnp.bfloat16)
    return (hidden, stream)
```

```python
import functools

import jax
import jax.numpy as jnp
from jax import lax
from jax.experimental import pallas as pl
from jax.experimental.pallas import tpu as pltpu
from jax.sharding import PartitionSpec as P

epsilon = 1e-06
CORES = 2
MESH = pl.DeviceIdType.MESH


def rms_scaled(values, gain):
    return values * lax.rsqrt(jnp.mean(values * values, axis=-1, keepdims=True) + epsilon) * gain


def snake(n, i):
    if n % 2:
        return i
    pair = lax.div(i, 2)
    return pair * 2 + lax.rem(lax.rem(i, 2) + pair, 2)


def kernel(
    n, tp, chunk, tile,
    tok_ref, gate_ref, up_ref, gate_scale_ref, up_scale_ref, out_ref,
    tokens, weights, acc, hidden,
    local_sem, ring_send, ring_recv, z_send, z_recv, mate_send, mate_recv, out_sem,
):
    levels = tp // CORES
    rows, width = tok_ref.shape
    depth, cols = gate_ref.shape
    pieces = cols // chunk
    tiles = tp * rows // tile

    fs_i, tp_i = lax.axis_index("fs"), lax.axis_index("tp")
    z, core = lax.div(tp_i, CORES), lax.rem(tp_i, CORES)
    mate = z * CORES + (CORES - 1 - core)
    place = snake(n, fs_i)
    right = snake(n, lax.rem(place + 1, n))
    left = snake(n, lax.rem(place + n - 1, n))
    ring_to = ((right, tp_i), (left, tp_i))

    barrier = pltpu.get_barrier_semaphore()

    def greet(fs_to, tp_to):
        pl.semaphore_signal(barrier, inc=1, device_id=(fs_to, tp_to), device_id_type=MESH)

    greet(right, tp_i)
    greet(left, tp_i)
    greet(fs_i, mate)
    pl.when(z > 0)(lambda: greet(fs_i, tp_i - CORES))
    pl.when(z < levels - 1)(lambda: greet(fs_i, tp_i + CORES))
    pl.semaphore_wait(barrier, 3 + jnp.where(z > 0, 1, 0) + jnp.where(z < levels - 1, 1, 0))

    own = (gate_ref, up_ref)

    def piece(c):
        return pl.ds(c * chunk, chunk)

    def ring(way, hop, c):
        src = own[way].at[:, piece(c)] if hop == 1 else weights.at[way, hop - 1, :, piece(c)]
        return pltpu.make_async_remote_copy(
            src_ref=src,
            dst_ref=weights.at[way, hop, :, piece(c)],
            send_sem=ring_send.at[way, hop - 1, c],
            recv_sem=ring_recv.at[way, hop - 1, c],
            device_id=ring_to[way],
            device_id_type=MESH,
        )

    def block(tp_of):
        return tokens.at[pl.ds(pl.multiple_of(tp_of * rows, rows), rows), :]

    def z_copy(way, distance, source):
        step = CORES if way == 0 else -CORES
        return pltpu.make_async_remote_copy(
            src_ref=tok_ref if distance == 1 else block(source),
            dst_ref=block(source),
            send_sem=z_send.at[way, distance - 1],
            recv_sem=z_recv.at[way, distance - 1],
            device_id=(fs_i, tp_i + step),
            device_id_type=MESH,
        )

    def mate_copy(index, source):
        return pltpu.make_async_remote_copy(
            src_ref=tok_ref if index == 0 else block(source),
            dst_ref=block(source),
            send_sem=mate_send.at[index],
            recv_sem=mate_recv.at[index],
            device_id=(fs_i, mate),
            device_id_type=MESH,
        )

    def mate_index(way, distance):
        return way * (levels - 1) + distance

    def has_source(way, distance):
        return z >= distance if way == 0 else z + distance < levels

    def has_next(way):
        return z < levels - 1 if way == 0 else z > 0

    def source_of(way, distance, tp_of):
        return tp_of - distance * CORES if way == 0 else tp_of + distance * CORES

    for c in range(pieces):
        for way in range(2):
            ring(way, 1, c).start()
    for way in range(2):
        pl.when(has_next(way))(lambda way=way: z_copy(way, 1, tp_i).start())
    mate_copy(0, tp_i).start()
    local = [
        pltpu.make_async_copy(tok_ref, block(tp_i), local_sem.at[0]),
        pltpu.make_async_copy(gate_ref, weights.at[0, 0], local_sem.at[1]),
        pltpu.make_async_copy(up_ref, weights.at[1, 0], local_sem.at[2]),
    ]
    for copy in local:
        copy.start()

    def ring_event(hop, c):
        for way in range(2):
            ring(way, hop, c).wait_recv()
            ring(way, hop + 1, c).start()

    def z_event(distance):
        for way in range(2):
            source = source_of(way, distance, tp_i)

            @pl.when(has_source(way, distance))
            def _():
                z_copy(way, distance, source).wait_recv()
                mate_copy(mate_index(way, distance), source).start()
                if distance < levels - 1:
                    pl.when(has_next(way))(lambda: z_copy(way, distance + 1, source).start())

    ratio = rows * width / (depth * chunk)
    events = [((hop - 1) * pieces + c + 1, functools.partial(ring_event, hop, c))
              for hop in range(1, n - 1) for c in range(pieces)]
    events += [(d * ratio + 0.5, functools.partial(z_event, d)) for d in range(1, levels)]
    for _, event in sorted(events, key=lambda e: e[0]):
        event()

    mate_copy(0, mate).wait_recv()
    for way in range(2):
        for d in range(1, levels):
            pl.when(has_source(way, d))(
                lambda way=way, d=d: mate_copy(mate_index(way, d), source_of(way, d, mate)).wait_recv()
            )
    for copy in local:
        copy.wait()

    def product(way, slot, c, m):
        back = slot if way == 0 else n - slot
        origin = snake(n, lax.rem(place + n - back, n))
        left_side = tokens[
            pl.ds(pl.multiple_of(m * tile, tile), tile),
            pl.ds(pl.multiple_of(origin * depth, depth), depth),
        ]
        right_side = weights[way, slot, :, pl.ds(pl.multiple_of(c * chunk, chunk), chunk)]
        return jnp.dot(left_side, right_side, preferred_element_type=jnp.float32)

    for way in range(2):
        def early(i, carry, way=way):
            c, m = lax.div(i, tiles), lax.rem(i, tiles)
            total = product(way, 0, c, m)
            for slot in range(1, n - 1):
                total += product(way, slot, c, m)
            acc[way, pl.ds(pl.multiple_of(m * tile, tile), tile), pl.ds(pl.multiple_of(c * chunk, chunk), chunk)] = total
            return carry

        lax.fori_loop(0, tiles * pieces, early, 0)

    def out_copy(c):
        return pltpu.make_async_copy(hidden.at[:, piece(c)], out_ref.at[:, piece(c)], out_sem.at[c])

    for c in range(pieces):
        for way in range(2):
            ring(way, n - 1, c).wait_recv()

        def late(m, carry, c=c):
            at = pl.ds(pl.multiple_of(m * tile, tile), tile)
            gate = (acc[0, at, piece(c)] + product(0, n - 1, c, m)) * gate_scale_ref[:, piece(c)]
            up = (acc[1, at, piece(c)] + product(1, n - 1, c, m)) * up_scale_ref[:, piece(c)]
            hidden[at, piece(c)] = (gate / (1.0 + jnp.exp(-gate)) * up).astype(hidden.dtype)
            return carry

        lax.fori_loop(0, tiles, late, 0)
        out_copy(c).start()

    for c in range(pieces):
        for hop in range(1, n):
            for way in range(2):
                ring(way, hop, c).wait_send()
    mate_copy(0, tp_i).wait_send()
    for way in range(2):
        for d in range(1, levels):
            @pl.when(has_source(way, d))
            def _():
                mate_copy(mate_index(way, d), source_of(way, d, tp_i)).wait_send()
        pl.when(has_next(way))(lambda way=way: z_copy(way, 1, tp_i).wait_send())
        for d in range(1, levels - 1):
            @pl.when(has_source(way, d))
            def _():
                pl.when(has_next(way))(
                    lambda: z_copy(way, d + 1, source_of(way, d, tp_i)).wait_send()
                )
    for c in range(pieces):
        out_copy(c).wait()


def solution(mesh):
    n, tp = mesh.shape["fs"], mesh.shape["tp"]

    def on_device(
        stream_in, mixer_out, mix_gain, pre_gain, gate_weight, up_weight, gate_scale, up_scale
    ):
        mixed = stream_in.astype(jnp.float32) + rms_scaled(mixer_out.astype(jnp.float32), mix_gain)
        stream = mixed.astype(jnp.bfloat16)
        normed = rms_scaled(stream.astype(jnp.float32), pre_gain).astype(jnp.bfloat16)
        gate_cast = gate_weight.astype(jnp.bfloat16)
        up_cast = up_weight.astype(jnp.bfloat16)
        rows, width = normed.shape
        depth, cols = gate_cast.shape
        chunk = 256 if cols % 256 == 0 else 128
        tall = tp * rows
        tile = 512 if tall % 512 == 0 else rows
        levels, pieces = tp // CORES, cols // chunk
        anywhere = pl.BlockSpec(memory_space=pl.ANY)
        vmem = pl.BlockSpec(memory_space=pltpu.VMEM)
        dma = pltpu.SemaphoreType.DMA
        hidden = pl.pallas_call(
            functools.partial(kernel, n, tp, chunk, tile),
            out_shape=jax.ShapeDtypeStruct((tall, cols), jnp.bfloat16),
            in_specs=[anywhere] * 3 + [vmem] * 2,
            out_specs=anywhere,
            scratch_shapes=[
                pltpu.VMEM((tall, width), jnp.bfloat16),
                pltpu.VMEM((2, n, depth, cols), jnp.bfloat16),
                pltpu.VMEM((2, tall, cols), jnp.float32),
                pltpu.VMEM((tall, cols), jnp.bfloat16),
                dma((3,)),
                dma((2, n - 1, pieces)),
                dma((2, n - 1, pieces)),
                dma((2, levels)),
                dma((2, levels)),
                dma((2 * levels,)),
                dma((2 * levels,)),
                dma((pieces,)),
            ],
            compiler_params=pltpu.CompilerParams(
                collective_id=0, has_side_effects=True, vmem_limit_bytes=60 * 1024 * 1024
            ),
        )(normed, gate_cast, up_cast, gate_scale.reshape(1, -1), up_scale.reshape(1, -1))
        return (hidden, stream)

    return jax.shard_map(
        on_device,
        mesh=mesh,
        in_specs=(
            P(("fs", "tp"), None),
            P(("fs", "tp"), None),
            P(),
            P(),
            P("fs", "tp"),
            P("fs", "tp"),
            P("tp"),
            P("tp"),
        ),
        out_specs=(P("fs", "tp"), P(("fs", "tp"), None)),
        check_vma=False,
    )
```

```python
import functools

import jax
import jax.numpy as jnp
from jax import lax
from jax.experimental import pallas as pl
from jax.experimental.pallas import tpu as pltpu
from jax.sharding import PartitionSpec as P

epsilon = 1e-06
CORES = 2
ROWS = 16
MESH = pl.DeviceIdType.MESH


def rms_scaled(values, gain):
    return values * lax.rsqrt(jnp.mean(values * values, axis=-1, keepdims=True) + epsilon) * gain


def snake(n, i):
    if n % 2:
        return i
    pair = lax.div(i, 2)
    return pair * 2 + lax.rem(lax.rem(i, 2) + pair, 2)


def kernel(
    n, tp, chunk, tile,
    stream_ref, mixer_ref, mix_gain_ref, pre_gain_ref, gate_ref, up_ref, gate_scale_ref, up_scale_ref,
    hidden, stream_out,
    tokens, weights, acc, wide, stream_in, mixer,
    row_sem, wide_sem, ring_send, ring_recv, z_send, z_recv, mate_send, mate_recv,
):
    levels = tp // CORES
    rows, width = stream_ref.shape
    depth, cols = gate_ref.shape
    pieces = cols // chunk
    strip = min(depth, 128)
    tiles = tp * rows // tile

    fs_i, tp_i = lax.axis_index("fs"), lax.axis_index("tp")
    z, core = lax.div(tp_i, CORES), lax.rem(tp_i, CORES)
    mate = z * CORES + (CORES - 1 - core)
    place = snake(n, fs_i)
    right = snake(n, lax.rem(place + 1, n))
    left = snake(n, lax.rem(place + n - 1, n))
    ring_to = ((right, tp_i), (left, tp_i))

    def piece(c):
        return pl.ds(c * chunk, chunk)

    source = (gate_ref, up_ref)

    def wide_copy(way, c):
        return pltpu.make_async_copy(
            source[way].at[:, piece(c)], wide.at[way, :, piece(c)], wide_sem.at[way, c]
        )

    row_copies = (
        pltpu.make_async_copy(stream_ref, stream_in, row_sem.at[0]),
        pltpu.make_async_copy(mixer_ref, mixer, row_sem.at[1]),
    )
    for way in range(2):
        wide_copy(way, 0).start()
    for copy in row_copies:
        copy.start()
    for c in range(1, pieces):
        for way in range(2):
            wide_copy(way, c).start()

    barrier = pltpu.get_barrier_semaphore()

    def greet(fs_to, tp_to):
        pl.semaphore_signal(barrier, inc=1, device_id=(fs_to, tp_to), device_id_type=MESH)

    greet(right, tp_i)
    greet(left, tp_i)
    greet(fs_i, mate)
    pl.when(z > 0)(lambda: greet(fs_i, tp_i - CORES))
    pl.when(z < levels - 1)(lambda: greet(fs_i, tp_i + CORES))

    def cast(c):
        for way in range(2):
            wide_copy(way, c).wait()

            def some(i, carry, way=way):
                at = pl.ds(pl.multiple_of(i * strip, strip), strip)
                weights[way, 0, at, piece(c)] = wide[way, at, piece(c)].astype(weights.dtype)
                return carry

            lax.fori_loop(0, depth // strip, some, 0)

    cast(0)
    pl.semaphore_wait(barrier, 3 + jnp.where(z > 0, 1, 0) + jnp.where(z < levels - 1, 1, 0))

    def ring(way, hop, c):
        return pltpu.make_async_remote_copy(
            src_ref=weights.at[way, hop - 1, :, piece(c)],
            dst_ref=weights.at[way, hop, :, piece(c)],
            send_sem=ring_send.at[way, hop - 1, c],
            recv_sem=ring_recv.at[way, hop - 1, c],
            device_id=ring_to[way],
            device_id_type=MESH,
        )

    def block(tp_of):
        return tokens.at[pl.ds(pl.multiple_of(tp_of * rows, rows), rows), :]

    def z_copy(way, distance, source):
        step = CORES if way == 0 else -CORES
        return pltpu.make_async_remote_copy(
            src_ref=block(source),
            dst_ref=block(source),
            send_sem=z_send.at[way, distance - 1],
            recv_sem=z_recv.at[way, distance - 1],
            device_id=(fs_i, tp_i + step),
            device_id_type=MESH,
        )

    def mate_copy(index, source):
        return pltpu.make_async_remote_copy(
            src_ref=block(source),
            dst_ref=block(source),
            send_sem=mate_send.at[index],
            recv_sem=mate_recv.at[index],
            device_id=(fs_i, mate),
            device_id_type=MESH,
        )

    def mate_index(way, distance):
        return way * (levels - 1) + distance

    def has_source(way, distance):
        return z >= distance if way == 0 else z + distance < levels

    def has_next(way):
        return z < levels - 1 if way == 0 else z > 0

    def source_of(way, distance, tp_of):
        return tp_of - distance * CORES if way == 0 else tp_of + distance * CORES

    for way in range(2):
        ring(way, 1, 0).start()

    for copy in row_copies:
        copy.wait()
    mix_gain, pre_gain = mix_gain_ref[...].reshape(1, -1), pre_gain_ref[...].reshape(1, -1)

    def norm(i, carry):
        at = pl.ds(pl.multiple_of(i * ROWS, ROWS), ROWS)
        mixed = stream_in[at, :].astype(jnp.float32) + rms_scaled(
            mixer[at, :].astype(jnp.float32), mix_gain
        )
        stream = mixed.astype(stream_out.dtype)
        stream_out[at, :] = stream
        own_at = pl.ds(pl.multiple_of(tp_i * rows + i * ROWS, ROWS), ROWS)
        tokens[own_at, :] = rms_scaled(stream.astype(jnp.float32), pre_gain).astype(tokens.dtype)
        return carry

    lax.fori_loop(0, rows // ROWS, norm, 0)
    for c in range(1, pieces):
        cast(c)
    for way in range(2):
        pl.when(has_next(way))(lambda way=way: z_copy(way, 1, tp_i).start())
    mate_copy(0, tp_i).start()
    for c in range(1, pieces):
        for way in range(2):
            ring(way, 1, c).start()

    def ring_event(hop, c):
        for way in range(2):
            ring(way, hop, c).wait_recv()
            ring(way, hop + 1, c).start()

    def z_event(distance):
        for way in range(2):
            source = source_of(way, distance, tp_i)

            @pl.when(has_source(way, distance))
            def _():
                z_copy(way, distance, source).wait_recv()
                mate_copy(mate_index(way, distance), source).start()
                if distance < levels - 1:
                    pl.when(has_next(way))(lambda: z_copy(way, distance + 1, source).start())

    ratio = rows * width / (depth * chunk)
    events = [((hop - 1) * pieces + c + 1, functools.partial(ring_event, hop, c))
              for hop in range(1, n - 1) for c in range(pieces)]
    events += [(d * ratio + 0.5, functools.partial(z_event, d)) for d in range(1, levels)]
    for _, event in sorted(events, key=lambda e: e[0]):
        event()

    mate_copy(0, mate).wait_recv()
    for way in range(2):
        for d in range(1, levels):
            pl.when(has_source(way, d))(
                lambda way=way, d=d: mate_copy(mate_index(way, d), source_of(way, d, mate)).wait_recv()
            )

    def product(way, slot, c, m):
        back = slot if way == 0 else n - slot
        origin = snake(n, lax.rem(place + n - back, n))
        left_side = tokens[
            pl.ds(pl.multiple_of(m * tile, tile), tile),
            pl.ds(pl.multiple_of(origin * depth, depth), depth),
        ]
        right_side = weights[way, slot, :, pl.ds(pl.multiple_of(c * chunk, chunk), chunk)]
        return jnp.dot(left_side, right_side, preferred_element_type=jnp.float32)

    for way in range(2):
        def early(i, carry, way=way):
            c, m = lax.div(i, tiles), lax.rem(i, tiles)
            total = product(way, 0, c, m)
            for slot in range(1, n - 1):
                total += product(way, slot, c, m)
            acc[way, pl.ds(pl.multiple_of(m * tile, tile), tile), pl.ds(pl.multiple_of(c * chunk, chunk), chunk)] = total
            return carry

        lax.fori_loop(0, tiles * pieces, early, 0)

    gate_scale, up_scale = gate_scale_ref[...].reshape(1, -1), up_scale_ref[...].reshape(1, -1)
    for c in range(pieces):
        for way in range(2):
            ring(way, n - 1, c).wait_recv()

        def late(m, carry, c=c):
            at = pl.ds(pl.multiple_of(m * tile, tile), tile)
            gate = (acc[0, at, piece(c)] + product(0, n - 1, c, m)) * gate_scale[:, c * chunk:(c + 1) * chunk]
            up = (acc[1, at, piece(c)] + product(1, n - 1, c, m)) * up_scale[:, c * chunk:(c + 1) * chunk]
            hidden[at, piece(c)] = (gate / (1.0 + jnp.exp(-gate)) * up).astype(hidden.dtype)
            return carry

        lax.fori_loop(0, tiles, late, 0)

    for c in range(pieces):
        for hop in range(1, n):
            for way in range(2):
                ring(way, hop, c).wait_send()
    mate_copy(0, tp_i).wait_send()
    for way in range(2):
        for d in range(1, levels):
            @pl.when(has_source(way, d))
            def _():
                mate_copy(mate_index(way, d), source_of(way, d, tp_i)).wait_send()
        pl.when(has_next(way))(lambda way=way: z_copy(way, 1, tp_i).wait_send())
        for d in range(1, levels - 1):
            @pl.when(has_source(way, d))
            def _():
                pl.when(has_next(way))(
                    lambda: z_copy(way, d + 1, source_of(way, d, tp_i)).wait_send()
                )


def solution(mesh):
    n, tp = mesh.shape["fs"], mesh.shape["tp"]

    def on_device(
        stream_in, mixer_out, mix_gain, pre_gain, gate_weight, up_weight, gate_scale, up_scale
    ):
        (rows, width), (depth, cols) = stream_in.shape, gate_weight.shape
        chunk = 256 if cols % 256 == 0 else 128
        tall = tp * rows
        tile = 512 if tall % 512 == 0 else rows
        levels, pieces = tp // CORES, cols // chunk
        anywhere = pl.BlockSpec(memory_space=pl.ANY)
        vmem = pl.BlockSpec(memory_space=pltpu.VMEM)
        dma = pltpu.SemaphoreType.DMA
        return pl.pallas_call(
            functools.partial(kernel, n, tp, chunk, tile),
            out_shape=(
                jax.ShapeDtypeStruct((tall, cols), jnp.bfloat16),
                jax.ShapeDtypeStruct((rows, width), jnp.bfloat16),
            ),
            in_specs=[anywhere] * 2 + [vmem] * 2 + [anywhere] * 2 + [vmem] * 2,
            out_specs=(vmem, vmem),
            scratch_shapes=[
                pltpu.VMEM((tall, width), jnp.bfloat16),
                pltpu.VMEM((2, n, depth, cols), jnp.bfloat16),
                pltpu.VMEM((2, tall, cols), jnp.float32),
                pltpu.VMEM((2, depth, cols), jnp.float32),
                pltpu.VMEM((rows, width), jnp.bfloat16),
                pltpu.VMEM((rows, width), jnp.bfloat16),
                dma((2,)),
                dma((2, pieces)),
                dma((2, n - 1, pieces)),
                dma((2, n - 1, pieces)),
                dma((2, levels)),
                dma((2, levels)),
                dma((2 * levels,)),
                dma((2 * levels,)),
            ],
            compiler_params=pltpu.CompilerParams(
                collective_id=0, has_side_effects=True, vmem_limit_bytes=48 * 1024 * 1024
            ),
        )(
            stream_in, mixer_out, mix_gain, pre_gain,
            gate_weight, up_weight, gate_scale, up_scale,
        )

    return jax.shard_map(
        on_device,
        mesh=mesh,
        in_specs=(
            P(("fs", "tp"), None),
            P(("fs", "tp"), None),
            P(),
            P(),
            P("fs", "tp"),
            P("fs", "tp"),
            P("tp"),
            P("tp"),
        ),
        out_specs=(P("fs", "tp"), P(("fs", "tp"), None)),
        check_vma=False,
    )
```

```python
import functools

import jax
import jax.numpy as jnp
from jax import lax
from jax.experimental import pallas as pl
from jax.experimental.pallas import tpu as pltpu
from jax.sharding import PartitionSpec as P

epsilon = 1e-06
CORES = 2
ROWS = 16
MESH = pl.DeviceIdType.MESH


def rms_scaled(values, gain):
    return values * lax.rsqrt(jnp.mean(values * values, axis=-1, keepdims=True) + epsilon) * gain


def snake(n, i):
    if n % 2:
        return i
    pair = lax.div(i, 2)
    return pair * 2 + lax.rem(lax.rem(i, 2) + pair, 2)


def kernel(
    n, tp, chunk, tile,
    stream_ref, mixer_ref, mix_gain_ref, pre_gain_ref, gate_ref, up_ref, gate_scale_ref, up_scale_ref,
    hidden, stream_out,
    tokens, weights, acc, wide, stream_in, mixer, gains, scales,
    row_sem, wide_sem, ring_send, ring_recv, z_send, z_recv, mate_send, mate_recv,
):
    levels = tp // CORES
    rows, width = stream_ref.shape
    depth, cols = gate_ref.shape
    pieces = cols // chunk
    strip = min(depth, 128)
    tiles = tp * rows // tile

    fs_i, tp_i = lax.axis_index("fs"), lax.axis_index("tp")
    z, core = lax.div(tp_i, CORES), lax.rem(tp_i, CORES)
    mate = z * CORES + (CORES - 1 - core)
    place = snake(n, fs_i)
    right = snake(n, lax.rem(place + 1, n))
    left = snake(n, lax.rem(place + n - 1, n))
    ring_to = ((right, tp_i), (left, tp_i))

    def piece(c):
        return pl.ds(c * chunk, chunk)

    source = (gate_ref, up_ref)

    def wide_copy(way, c):
        return pltpu.make_async_copy(
            source[way].at[:, piece(c)], wide.at[way, :, piece(c)], wide_sem.at[way, c]
        )

    row_copies = (
        pltpu.make_async_copy(stream_ref, stream_in, row_sem.at[0]),
        pltpu.make_async_copy(mixer_ref, mixer, row_sem.at[1]),
        pltpu.make_async_copy(mix_gain_ref, gains[0], row_sem.at[2]),
        pltpu.make_async_copy(pre_gain_ref, gains[1], row_sem.at[3]),
        pltpu.make_async_copy(gate_scale_ref, scales[0], row_sem.at[4]),
        pltpu.make_async_copy(up_scale_ref, scales[1], row_sem.at[5]),
    )
    for way in range(2):
        wide_copy(way, 0).start()
    for copy in row_copies:
        copy.start()
    for c in range(1, pieces):
        for way in range(2):
            wide_copy(way, c).start()

    barrier = pltpu.get_barrier_semaphore()

    def greet(fs_to, tp_to):
        pl.semaphore_signal(barrier, inc=1, device_id=(fs_to, tp_to), device_id_type=MESH)

    greet(right, tp_i)
    greet(left, tp_i)
    greet(fs_i, mate)
    pl.when(z > 0)(lambda: greet(fs_i, tp_i - CORES))
    pl.when(z < levels - 1)(lambda: greet(fs_i, tp_i + CORES))

    def cast(c):
        for way in range(2):
            wide_copy(way, c).wait()

            def some(i, carry, way=way):
                at = pl.ds(pl.multiple_of(i * strip, strip), strip)
                weights[way, 0, at, piece(c)] = wide[way, at, piece(c)].astype(weights.dtype)
                return carry

            lax.fori_loop(0, depth // strip, some, 0)

    cast(0)
    pl.semaphore_wait(barrier, 3 + jnp.where(z > 0, 1, 0) + jnp.where(z < levels - 1, 1, 0))

    def ring(way, hop, c):
        return pltpu.make_async_remote_copy(
            src_ref=weights.at[way, hop - 1, :, piece(c)],
            dst_ref=weights.at[way, hop, :, piece(c)],
            send_sem=ring_send.at[way, hop - 1, c],
            recv_sem=ring_recv.at[way, hop - 1, c],
            device_id=ring_to[way],
            device_id_type=MESH,
        )

    def block(tp_of):
        return tokens.at[pl.ds(pl.multiple_of(tp_of * rows, rows), rows), :]

    def z_copy(way, distance, source):
        step = CORES if way == 0 else -CORES
        return pltpu.make_async_remote_copy(
            src_ref=block(source),
            dst_ref=block(source),
            send_sem=z_send.at[way, distance - 1],
            recv_sem=z_recv.at[way, distance - 1],
            device_id=(fs_i, tp_i + step),
            device_id_type=MESH,
        )

    def mate_copy(index, source):
        return pltpu.make_async_remote_copy(
            src_ref=block(source),
            dst_ref=block(source),
            send_sem=mate_send.at[index],
            recv_sem=mate_recv.at[index],
            device_id=(fs_i, mate),
            device_id_type=MESH,
        )

    def mate_index(way, distance):
        return way * (levels - 1) + distance

    def has_source(way, distance):
        return z >= distance if way == 0 else z + distance < levels

    def has_next(way):
        return z < levels - 1 if way == 0 else z > 0

    def source_of(way, distance, tp_of):
        return tp_of - distance * CORES if way == 0 else tp_of + distance * CORES

    for way in range(2):
        ring(way, 1, 0).start()

    for copy in row_copies:
        copy.wait()
    mix_gain, pre_gain = (gain[...].reshape(1, -1) for gain in gains)

    def norm(i, carry):
        at = pl.ds(pl.multiple_of(i * ROWS, ROWS), ROWS)
        mixed = stream_in[at, :].astype(jnp.float32) + rms_scaled(
            mixer[at, :].astype(jnp.float32), mix_gain
        )
        stream = mixed.astype(stream_out.dtype)
        stream_out[at, :] = stream
        own_at = pl.ds(pl.multiple_of(tp_i * rows + i * ROWS, ROWS), ROWS)
        tokens[own_at, :] = rms_scaled(stream.astype(jnp.float32), pre_gain).astype(tokens.dtype)
        return carry

    lax.fori_loop(0, rows // ROWS, norm, 0)
    for c in range(1, pieces):
        cast(c)
    for way in range(2):
        pl.when(has_next(way))(lambda way=way: z_copy(way, 1, tp_i).start())
    mate_copy(0, tp_i).start()
    for c in range(1, pieces):
        for way in range(2):
            ring(way, 1, c).start()

    def ring_event(hop, c):
        for way in range(2):
            ring(way, hop, c).wait_recv()
            ring(way, hop + 1, c).start()

    def z_event(distance):
        for way in range(2):
            source = source_of(way, distance, tp_i)

            @pl.when(has_source(way, distance))
            def _():
                z_copy(way, distance, source).wait_recv()
                mate_copy(mate_index(way, distance), source).start()
                if distance < levels - 1:
                    pl.when(has_next(way))(lambda: z_copy(way, distance + 1, source).start())

    ratio = rows * width / (depth * chunk)
    events = [((hop - 1) * pieces + c + 1, functools.partial(ring_event, hop, c))
              for hop in range(1, n - 1) for c in range(pieces)]
    events += [(d * ratio + 0.5, functools.partial(z_event, d)) for d in range(1, levels)]
    for _, event in sorted(events, key=lambda e: e[0]):
        event()

    mate_copy(0, mate).wait_recv()
    for way in range(2):
        for d in range(1, levels):
            pl.when(has_source(way, d))(
                lambda way=way, d=d: mate_copy(mate_index(way, d), source_of(way, d, mate)).wait_recv()
            )

    def product(way, slot, c, m):
        back = slot if way == 0 else n - slot
        origin = snake(n, lax.rem(place + n - back, n))
        left_side = tokens[
            pl.ds(pl.multiple_of(m * tile, tile), tile),
            pl.ds(pl.multiple_of(origin * depth, depth), depth),
        ]
        right_side = weights[way, slot, :, pl.ds(pl.multiple_of(c * chunk, chunk), chunk)]
        return jnp.dot(left_side, right_side, preferred_element_type=jnp.float32)

    for way in range(2):
        def early(i, carry, way=way):
            c, m = lax.div(i, tiles), lax.rem(i, tiles)
            total = product(way, 0, c, m)
            for slot in range(1, n - 1):
                total += product(way, slot, c, m)
            acc[way, pl.ds(pl.multiple_of(m * tile, tile), tile), pl.ds(pl.multiple_of(c * chunk, chunk), chunk)] = total
            return carry

        lax.fori_loop(0, tiles * pieces, early, 0)

    gate_scale, up_scale = (scale[...].reshape(1, -1) for scale in scales)
    for c in range(pieces):
        for way in range(2):
            ring(way, n - 1, c).wait_recv()

        def late(m, carry, c=c):
            at = pl.ds(pl.multiple_of(m * tile, tile), tile)
            gate = (acc[0, at, piece(c)] + product(0, n - 1, c, m)) * gate_scale[:, c * chunk:(c + 1) * chunk]
            up = (acc[1, at, piece(c)] + product(1, n - 1, c, m)) * up_scale[:, c * chunk:(c + 1) * chunk]
            hidden[at, piece(c)] = (gate / (1.0 + jnp.exp(-gate)) * up).astype(hidden.dtype)
            return carry

        lax.fori_loop(0, tiles, late, 0)

    for c in range(pieces):
        for hop in range(1, n):
            for way in range(2):
                ring(way, hop, c).wait_send()
    mate_copy(0, tp_i).wait_send()
    for way in range(2):
        for d in range(1, levels):
            @pl.when(has_source(way, d))
            def _():
                mate_copy(mate_index(way, d), source_of(way, d, tp_i)).wait_send()
        pl.when(has_next(way))(lambda way=way: z_copy(way, 1, tp_i).wait_send())
        for d in range(1, levels - 1):
            @pl.when(has_source(way, d))
            def _():
                pl.when(has_next(way))(
                    lambda: z_copy(way, d + 1, source_of(way, d, tp_i)).wait_send()
                )


def solution(mesh):
    n, tp = mesh.shape["fs"], mesh.shape["tp"]

    def on_device(
        stream_in, mixer_out, mix_gain, pre_gain, gate_weight, up_weight, gate_scale, up_scale
    ):
        (rows, width), (depth, cols) = stream_in.shape, gate_weight.shape
        chunk = 256 if cols % 256 == 0 else 128
        tall = tp * rows
        tile = 512 if tall % 512 == 0 else rows
        levels, pieces = tp // CORES, cols // chunk
        hbm = pl.BlockSpec(memory_space=pltpu.HBM)
        vmem = pl.BlockSpec(memory_space=pltpu.VMEM)
        dma = pltpu.SemaphoreType.DMA
        return pl.pallas_call(
            functools.partial(kernel, n, tp, chunk, tile),
            out_shape=(
                jax.ShapeDtypeStruct((tall, cols), jnp.bfloat16),
                jax.ShapeDtypeStruct((rows, width), jnp.bfloat16),
            ),
            in_specs=[hbm] * 8,
            out_specs=(vmem, vmem),
            scratch_shapes=[
                pltpu.VMEM((tall, width), jnp.bfloat16),
                pltpu.VMEM((2, n, depth, cols), jnp.bfloat16),
                pltpu.VMEM((2, tall, cols), jnp.float32),
                pltpu.VMEM((2, depth, cols), jnp.float32),
                pltpu.VMEM((rows, width), jnp.bfloat16),
                pltpu.VMEM((rows, width), jnp.bfloat16),
                (pltpu.VMEM((width,), jnp.float32),) * 2,
                (pltpu.VMEM((cols,), jnp.float32),) * 2,
                dma((6,)),
                dma((2, pieces)),
                dma((2, n - 1, pieces)),
                dma((2, n - 1, pieces)),
                dma((2, levels)),
                dma((2, levels)),
                dma((2 * levels,)),
                dma((2 * levels,)),
            ],
            compiler_params=pltpu.CompilerParams(
                collective_id=0, has_side_effects=True, vmem_limit_bytes=57 * 1024 * 1024
            ),
        )(
            stream_in, mixer_out, mix_gain, pre_gain,
            gate_weight, up_weight, gate_scale, up_scale,
        )

    return jax.shard_map(
        on_device,
        mesh=mesh,
        in_specs=(
            P(("fs", "tp"), None),
            P(("fs", "tp"), None),
            P(),
            P(),
            P("fs", "tp"),
            P("fs", "tp"),
            P("tp"),
            P("tp"),
        ),
        out_specs=(P("fs", "tp"), P(("fs", "tp"), None)),
        check_vma=False,
    )
```
